32 devices in a mesh: kv: 8 (over z, y), tp: 4 (over x, core).
Axes of the slice: x: 2, y: 2, z: 4, core: 2. Of those that a mesh axis runs over, the one named last changes fastest.
Arguments:
- residual_in: bfloat16 [64, 2048], P(None, ('kv', 'tp')), may hold values from -14 to 14
- delta_state: float32 [64, 32, 128, 128], P('kv', 'tp'), may hold values from -1 to 1
- norm_gain_first: float32 [2048], P('kv'), may hold values from 0.1 to 1.9
- gate_first: bfloat16 [2048, 5632], P('kv', 'tp'), may hold values from -0.125 to 0.125
- up_first: bfloat16 [2048, 5632], P('kv', 'tp'), may hold values from -0.125 to 0.125
- down_first: bfloat16 [5632, 2048], P('tp', 'kv'), may hold values from -0.15625 to 0.15625
- norm_gain_mixer: float32 [2048], P('kv'), may hold values from 0.1 to 1.9
- query_weight: bfloat16 [2048, 2048], P('kv', 'tp'), may hold values from -0.125 to 0.125
- key_weight: bfloat16 [2048, 2048], P('kv', 'tp'), may hold values from -0.125 to 0.125
- value_weight: bfloat16 [2048, 4096], P('kv', 'tp'), may hold values from -0.125 to 0.125
- output_gate_weight: bfloat16 [2048, 4096], P('kv', 'tp'), may hold values from -0.125 to 0.125
- beta_weight: bfloat16 [2048, 32], P('kv'), may hold values from -0.125 to 0.125
- decay_weight: bfloat16 [2048, 32], P('kv'), may hold values from -0.125 to 0.125
- decay_rate: float32 [32], P('tp'), may hold values from -2.3 to 1.1
- decay_bias: float32 [32], P('tp'), may hold values from -1 to 1
- head_gain: float32 [128], replicated, may hold values from 0.1 to 1.9
- out_weight: bfloat16 [4096, 2048], P('tp', 'kv'), may hold values from -0.125 to 0.125
- norm_gain_second: float32 [2048], P('kv'), may hold values from 0.1 to 1.9
- gate_second: bfloat16 [2048, 5632], P('kv', 'tp'), may hold values from -0.125 to 0.125
- up_second: bfloat16 [2048, 5632], P('kv', 'tp'), may hold values from -0.125 to 0.125
- down_second: bfloat16 [5632, 2048], P('tp', 'kv'), may hold values from -0.15625 to 0.15625
Outputs:
- residual_out: bfloat16 [64, 2048], P(None, ('kv', 'tp'))
- delta_state_out: float32 [64, 32, 128, 128], P('kv', 'tp')
The draws below stay inside these ranges and needn't reach their ends.
All inputs are finite; a program needn't handle non-finite values.
Results may differ from the reference program's by a relative error of at most 0.03.
Values may be sent and summed in bfloat16 or wider, within the bound.
A program may use at most 64 MiB of HBM per device.

```python
import jax
import jax.numpy as jnp
from jax import lax

D = 2048
FF = 5632
K_HEADS = 16
HEAD = 128
V_HEADS = 32
KW = 2048
VW = 4096
BATCH = 64
N_TP = 4


def draw_residual_in(key, part):
    keys = jax.random.split(key, 4)
    region = jnp.arange(D, dtype=jnp.int32) // (D // 8)
    region_scale = jnp.exp(jax.random.uniform(keys[0], (8,), jnp.float32, -0.6, 0.6))
    column_scale = region_scale[region] * jnp.exp(jax.random.uniform(keys[1], (D,), jnp.float32, -0.2, 0.2))
    base = jnp.clip(jax.random.normal(keys[2], (BATCH, D), jnp.float32), -4.0, 4.0)
    row_scale = jnp.exp(jax.random.uniform(keys[3], (BATCH, 1), jnp.float32, -0.4, 0.4))
    return (base * row_scale * column_scale[None, :]).astype(jnp.bfloat16)


def shard_levels(own_key, dims, cuts, smallest, largest):
    loudness, own = 1.0, jax.random.fold_in(own_key, 6)
    for dim, shards_of in cuts:
        draws = jnp.exp(jax.random.uniform(jax.random.fold_in(own, dim), (shards_of,), jnp.float32, smallest / len(cuts), largest / len(cuts)))
        loudness = loudness * jnp.repeat(draws, dims[dim] // shards_of).reshape([-1 if axis == dim else 1 for axis in range(len(dims))])
    return loudness


def bell_draw(rng, dims, spread, reach, cuts=(), kind=jnp.bfloat16):
    factor_of = shard_levels(rng, dims, cuts, -0.22, 0.18) if cuts else 1.0
    result = jax.random.normal(rng, dims, jnp.float32) * spread * factor_of
    return jnp.minimum(jnp.maximum(result, -reach), reach).astype(kind)


def setup_inputs(seed: int = 0) -> dict:
    key_list = jax.random.split(jax.random.key(seed), 22)
    return {
        "residual_in": draw_residual_in(jax.random.fold_in(key_list[21], 71), 0),
        "delta_state": bell_draw(key_list[1], (BATCH, V_HEADS, HEAD, HEAD), 0.2, 1.0, ((0, 8), (1, 4)), jnp.float32),
        "norm_gain_first": jnp.clip(1.0 + 0.18 * jax.random.normal(key_list[2], (D,), jnp.float32), 0.1, 1.9),
        "gate_first": bell_draw(key_list[3], (D, FF), D ** -0.5, 0.125, ((0, 8), (1, 4))),
        "up_first": bell_draw(key_list[4], (D, FF), D ** -0.5, 0.125, ((0, 8), (1, 4))),
        "down_first": bell_draw(key_list[5], (FF, D), (FF // 4) ** -0.5, 0.15625, ((0, 4), (1, 8))),
        "norm_gain_mixer": jnp.clip(1.0 + 0.18 * jax.random.normal(key_list[6], (D,), jnp.float32), 0.1, 1.9),
        "query_weight": bell_draw(key_list[7], (D, KW), D ** -0.5, 0.125, ((0, 8), (1, 4))),
        "key_weight": bell_draw(key_list[8], (D, KW), D ** -0.5, 0.125, ((0, 8), (1, 4))),
        "value_weight": bell_draw(key_list[9], (D, VW), D ** -0.5, 0.125, ((0, 8), (1, 4))),
        "output_gate_weight": bell_draw(key_list[10], (D, VW), D ** -0.5, 0.125, ((0, 8), (1, 4))),
        "beta_weight": bell_draw(key_list[11], (D, V_HEADS), D ** -0.5, 0.125, ((0, 8),)),
        "decay_weight": bell_draw(key_list[12], (D, V_HEADS), D ** -0.5, 0.125, ((0, 8),)),
        "decay_rate": jnp.clip(-2.3 + 3.4 * jax.random.uniform(key_list[13], (V_HEADS,), jnp.float32) ** shard_levels(key_list[13], (V_HEADS,), ((0, 4),), -0.2, 0.2), -2.3, 1.1),
        "decay_bias": jnp.clip(jax.random.uniform(key_list[14], (V_HEADS,), jnp.float32, -1.0, 1.0) * shard_levels(key_list[14], (V_HEADS,), ((0, 4),), -0.4, 0.0), -1.0, 1.0),
        "head_gain": jnp.clip(1.0 + 0.18 * jax.random.normal(key_list[15], (HEAD,), jnp.float32), 0.1, 1.9),
        "out_weight": bell_draw(key_list[16], (VW, D), (VW // 2) ** -0.5, 0.125, ((0, 4), (1, 8))),
        "norm_gain_second": jnp.clip(1.0 + 0.18 * jax.random.normal(key_list[17], (D,), jnp.float32), 0.1, 1.9),
        "gate_second": bell_draw(key_list[18], (D, FF), D ** -0.5, 0.125, ((0, 8), (1, 4))),
        "up_second": bell_draw(key_list[19], (D, FF), D ** -0.5, 0.125, ((0, 8), (1, 4))),
        "down_second": bell_draw(key_list[20], (FF, D), (FF // 4) ** -0.5, 0.15625, ((0, 4), (1, 8))),
    }


epsilon = 1e-06

def head_sums(left_side, right_side):
    left_parts = left_side.reshape(left_side.shape[0], N_TP, -1).astype(jnp.float32)
    weights = right_side.reshape(N_TP, -1, right_side.shape[1]).astype(jnp.float32)
    pieces = jnp.einsum('btf,tfd->tbd', left_parts, weights)
    rounded = lax.optimization_barrier(pieces.astype(jnp.bfloat16))
    return lax.optimization_barrier(jnp.sum(rounded.astype(jnp.float32), axis=0))

def norm_parts(residual, norm_gain):
    as_float = residual.astype(jnp.float32)
    rowscale = lax.rsqrt(lax.optimization_barrier(jnp.sum(as_float * as_float, axis=1, keepdims=True)) / D + epsilon)
    scaled = (as_float * norm_gain).astype(jnp.bfloat16)
    return (as_float, rowscale, scaled)

def half_ffn(residual, norm_gain, gate_weight, up_weight, down_weight):
    as_float, rowscale, scaled = norm_parts(residual, norm_gain)
    gate_act = jnp.dot(scaled, gate_weight, preferred_element_type=jnp.float32) * rowscale
    up_act = jnp.dot(scaled, up_weight, preferred_element_type=jnp.float32) * rowscale
    hidden = (jax.nn.silu(gate_act) * up_act).astype(jnp.bfloat16)
    branch = head_sums(hidden, down_weight)
    return (as_float + 0.5 * branch).astype(jnp.bfloat16)

def unit_heads(projected, head_size):
    activated = jax.nn.silu(projected).reshape(projected.shape[0], -1, head_size)
    return activated * lax.rsqrt(lax.optimization_barrier(jnp.sum(activated * activated, axis=-1, keepdims=True)) + epsilon)

def delta_step(old_state, key_rows, queries, values, beta_gate, decay_gate):
    faded_state = old_state * decay_gate[:, :, None, None]
    predicted = jnp.einsum('rhab,rha->rhb', faded_state, key_rows, precision=lax.Precision.HIGHEST)
    correction = beta_gate[:, :, None] * (values - predicted)
    updated = faded_state + key_rows[:, :, :, None] * correction[:, :, None, :]
    reading = jnp.einsum('rhab,rha->rhb', updated, queries, precision=lax.Precision.HIGHEST)
    return (updated, reading)

def advance(inputs):
    return delta_step(*inputs)

def reference(residual_in, delta_state, norm_gain_first, gate_first, up_first, down_first, norm_gain_mixer, query_weight, key_weight, value_weight, output_gate_weight, beta_weight, decay_weight, decay_rate, decay_bias, head_gain, out_weight, norm_gain_second, gate_second, up_second, down_second):
    after_first = half_ffn(residual_in, norm_gain_first, gate_first, up_first, down_first)
    as_float, rowscale, scaled = norm_parts(after_first, norm_gain_mixer)

    def project(weight):
        return jnp.dot(scaled, weight, preferred_element_type=jnp.float32) * rowscale
    repeat_count = V_HEADS // K_HEADS
    queries = jnp.repeat(unit_heads(project(query_weight), HEAD) * HEAD ** (-0.5), repeat_count, axis=1)
    key_rows = jnp.repeat(unit_heads(project(key_weight), HEAD), repeat_count, axis=1)
    values = jax.nn.silu(project(value_weight)).reshape(BATCH, V_HEADS, HEAD)
    out_gate = jax.nn.silu(project(output_gate_weight)).reshape(BATCH, V_HEADS, HEAD)
    beta_gate = jax.nn.sigmoid(project(beta_weight))
    decay_gate = jnp.exp(-jnp.exp(decay_rate)[None, :] * jax.nn.softplus(project(decay_weight) + decay_bias[None, :]))
    groups = BATCH // 8
    stacked = tuple((item.reshape((groups, BATCH // groups) + item.shape[1:]) for item in (delta_state, key_rows, queries, values, beta_gate, decay_gate)))
    new_state, reading = lax.map(advance, stacked)
    new_state = new_state.reshape(BATCH, V_HEADS, HEAD, HEAD)
    reading = reading.reshape(BATCH, V_HEADS, HEAD)
    normed = reading * lax.rsqrt(lax.optimization_barrier(jnp.mean(reading * reading, axis=-1, keepdims=True)) + epsilon)
    normed = (normed * head_gain * out_gate).reshape(BATCH, VW).astype(jnp.bfloat16)
    after_mixer = (as_float + head_sums(normed, out_weight)).astype(jnp.bfloat16)
    residual_out = half_ffn(after_mixer, norm_gain_second, gate_second, up_second, down_second)
    return (residual_out, new_state)
```

```python
import functools

import jax
import jax.numpy as jnp
from jax import lax
from jax.experimental import pallas as pl
from jax.experimental.pallas import tpu as pltpu
from jax.sharding import PartitionSpec as P

EPS = 1e-06
LANES = 128
BF16 = jnp.bfloat16
F32 = jnp.float32


def pad_lanes(size):
    return -(-size // LANES) * LANES


def silu(v):
    return v / (1.0 + jnp.exp(-v))


def dot(a, b):
    return jnp.dot(a, b, preferred_element_type=F32)


def place(rows, cols, shift):
    row = lax.broadcasted_iota(jnp.int32, (rows, cols), 0)
    col = lax.broadcasted_iota(jnp.int32, (rows, cols), 1)
    return jnp.where(col == row + shift, 1.0, 0.0).astype(F32).astype(BF16)


def kernel(
    n_kv,
    n_tp,
    res_ref,
    gain_first_ref,
    gain_mixer_ref,
    gain_second_ref,
    beta_ref,
    decay_ref,
    rate_ref,
    bias_ref,
    head_gain_ref,
    state_hbm,
    gate1_hbm,
    up1_hbm,
    down1_hbm,
    wq_hbm,
    wk_hbm,
    wv_hbm,
    wo_hbm,
    out_hbm,
    gate2_hbm,
    up2_hbm,
    down2_hbm,
    res_out_ref,
    state_out_hbm,
    gate1,
    up1,
    down1,
    wq,
    wk,
    wv,
    wo,
    wout,
    gate2,
    up2,
    down2,
    state,
    res_all,
    s1a,
    r1a,
    s1b,
    r1b,
    hid1,
    par1,
    sma,
    rma,
    smb,
    rmb,
    smc,
    rmc,
    nrm,
    parm,
    s2a,
    r2a,
    s2b,
    r2b,
    hid2,
    par2,
    qk_rows,
    val_rows,
    beta_rows,
    dec_rows,
    read_rows,
    w_sem,
    in_sem,
    out_sem,
    send_sem,
    recv_sem,
):
    kv = lax.axis_index("kv")
    tp = lax.axis_index("tp")
    batch, piece = res_ref.shape
    depth = gate1.shape[0]
    width = depth * n_kv
    own_rows = batch // n_kv
    heads = state.shape[1]
    size = state.shape[2]
    key_cols = wq.shape[1]
    key_heads = key_cols // size
    repeat = heads // key_heads
    val_cols = wv.shape[1]

    weight_pairs = (
        (gate1_hbm, gate1),
        (up1_hbm, up1),
        (down1_hbm, down1),
        (wq_hbm, wq),
        (wk_hbm, wk),
        (wv_hbm, wv),
        (wo_hbm, wo),
        (out_hbm, wout),
        (gate2_hbm, gate2),
        (up2_hbm, up2),
        (down2_hbm, down2),
    )
    loads = [
        pltpu.make_async_copy(src, dst, w_sem.at[i]) for i, (src, dst) in enumerate(weight_pairs)
    ]
    for load in loads[:7]:
        load.start()

    barrier = pltpu.get_barrier_semaphore()
    for off in range(1, n_tp):
        pl.semaphore_signal(
            barrier,
            inc=1,
            device_id={"tp": lax.rem(tp + off, n_tp)},
            device_id_type=pl.DeviceIdType.MESH,
        )
    for off in range(1, n_kv):
        pl.semaphore_signal(
            barrier,
            inc=1,
            device_id={"kv": lax.rem(kv + off, n_kv)},
            device_id_type=pl.DeviceIdType.MESH,
        )
    pl.semaphore_wait(barrier, n_tp - 1 + n_kv - 1)

    pending = []

    def send(event, off, src, dst, axis, peer):
        copy = pltpu.make_async_remote_copy(
            src_ref=src,
            dst_ref=dst,
            send_sem=send_sem.at[event, off],
            recv_sem=recv_sem.at[event, off],
            device_id={axis: peer},
            device_id_type=pl.DeviceIdType.MESH,
        )
        copy.start()
        pending.append(copy)
        return copy

    def gather(event, axis, me, count, own, slots):
        return [
            send(event, off, own, slots.at[me], axis, lax.rem(me + off, count))
            for off in range(1, count)
        ]

    def scatter(event, sends, receives):
        copies = []
        for off in range(1, n_kv):
            peer = lax.rem(kv + off, n_kv)
            copies.append(send(event, off, sends.at[peer], receives.at[kv], "kv", peer))
        return copies

    def collect(copies, sends, receives):
        total = sends[kv].astype(F32)
        for off in range(1, n_kv):
            copies[off - 1].wait_recv()
            source = lax.rem(kv + n_kv - off, n_kv)
            total = total + receives[source].astype(F32)
        return total

    def put(ref, offset, value):
        cols = value.shape[1]
        ref[:, :, offset : offset + cols] = value.reshape(n_kv, own_rows, cols).astype(BF16)

    def square_lanes(residual):
        squares = jnp.sum(residual * residual, axis=1, keepdims=True)
        high = squares.astype(BF16).astype(F32)
        lane = lax.broadcasted_iota(jnp.int32, (batch, LANES), 1)
        return jnp.where(lane == 64, high, jnp.where(lane == 65, squares - high, 0.0))

    def row_scale(extra):
        squares = extra[:, 64:65] + extra[:, 65:66]
        return lax.rsqrt(squares / width + EPS)

    def flat(slots):
        both = slots[...].astype(F32)
        return both.reshape(batch, both.shape[2]).astype(BF16)

    def exchange(event, value, slots):
        slots[tp] = value.astype(BF16)
        copies = gather(event, "tp", tp, n_tp, slots.at[tp], slots)
        for copy in copies:
            copy.wait_recv()
        total = slots[0].astype(F32)
        for other in range(1, n_tp):
            total = total + slots[other].astype(F32)
        return total

    def half_ffn(event, residual, gain_ref, first, w_gate, w_up, w_down, bufs, hid, par):
        send_a, recv_a, send_b, recv_b = bufs
        hidden_cols = w_gate.shape[1]
        up_end = pad_lanes(hidden_cols)
        scaled = (residual * gain_ref[...]).astype(BF16)
        loads[first].wait()
        put(send_a, 0, dot(scaled, w_gate[...]))
        copies_a = scatter(event, send_a, recv_a)
        loads[first + 1].wait()
        put(send_b, 0, dot(scaled, w_up[...]))
        put(send_b, up_end, square_lanes(residual))
        copies_b = scatter(event + 1, send_b, recv_b)
        gate_sum = collect(copies_a, send_a, recv_a)[:, :hidden_cols]
        rest = collect(copies_b, send_b, recv_b)
        scale = row_scale(rest[:, up_end:])
        hidden = (silu(gate_sum * scale) * (rest[:, :hidden_cols] * scale)).astype(BF16)
        hid[kv] = hidden
        copies = gather(event + 2, "kv", kv, n_kv, hid.at[kv], hid)
        loads[first + 2].wait()
        for copy in copies:
            copy.wait_recv()
        branch = exchange(event + 3, dot(flat(hid), w_down[...]), par)
        return (residual + 0.5 * branch).astype(BF16)

    copies = gather(0, "tp", tp, n_tp, res_ref, res_all)
    for load in loads[7:]:
        load.start()
    for row in range(own_rows):
        pltpu.make_async_copy(state_hbm.at[row], state.at[row], in_sem.at[row]).start()
    decay_exp = jnp.exp(rate_ref[...])
    extra_weight = (
        dot(beta_ref[...], place_heads(beta_ref.shape[1], tp * heads, 0, heads))
        + dot(decay_ref[...], place_heads(beta_ref.shape[1], tp * heads, heads, heads))
    ).astype(BF16)
    residual = dot(res_ref[...], place(piece, depth, tp * piece))
    for off in range(1, n_tp):
        copies[off - 1].wait_recv()
        source = lax.rem(tp + n_tp - off, n_tp)
        residual = residual + dot(res_all[source], place(piece, depth, source * piece))

    after_first = half_ffn(
        1, residual, gain_first_ref, 0, gate1, up1, down1, (s1a, r1a, s1b, r1b), hid1, par1
    ).astype(F32)

    scaled = (after_first * gain_mixer_ref[...]).astype(BF16)
    loads[3].wait()
    put(sma, 0, dot(scaled, wq[...]))
    loads[4].wait()
    put(sma, key_cols, dot(scaled, wk[...]))
    put(sma, 2 * key_cols, dot(scaled, extra_weight) + square_lanes(after_first))
    copies_a = scatter(5, sma, rma)
    loads[5].wait()
    put(smb, 0, dot(scaled, wv[...]))
    copies_b = scatter(6, smb, rmb)
    loads[6].wait()
    put(smc, 0, dot(scaled, wo[...]))
    copies_c = scatter(7, smc, rmc)

    keys_sum = collect(copies_a, sma, rma)
    extra = keys_sum[:, 2 * key_cols :]
    scale = row_scale(extra)
    for head in range(key_heads):
        for slot, start, factor in (
            (head, head * size, size ** (-0.5)),
            (key_heads + head, key_cols + head * size, 1.0),
        ):
            act = silu(keys_sum[:, start : start + size] * scale)
            unit = act * lax.rsqrt(jnp.sum(act * act, axis=1, keepdims=True) + EPS)
            qk_rows[:, slot, :] = unit * factor
    gates = extra * scale
    beta_pre = gates[:, :heads]
    decay_pre = gates[:, heads : 2 * heads] + bias_ref[...]
    beta_gate = 1.0 / (1.0 + jnp.exp(-beta_pre))
    softplus = jnp.maximum(decay_pre, 0.0) + jnp.log1p(jnp.exp(-jnp.abs(decay_pre)))
    decay_gate = jnp.exp(-decay_exp * softplus)
    for head in range(heads):
        beta_rows[:, head, :] = jnp.broadcast_to(beta_gate[:, head : head + 1], (own_rows, size))
        dec_rows[:, head, :] = jnp.broadcast_to(decay_gate[:, head : head + 1], (own_rows, size))
    values = silu(collect(copies_b, smb, rmb) * scale)
    for head in range(heads):
        val_rows[:, head, :] = values[:, head * size : (head + 1) * size]

    def step(row, carry):
        pltpu.make_async_copy(state_hbm.at[row], state.at[row], in_sem.at[row]).wait()
        columns = qk_rows[row].T
        row_vals, row_beta, row_dec = val_rows[row], beta_rows[row], dec_rows[row]
        for head in range(heads):
            kh = head // repeat
            key_col = columns[:, key_heads + kh : key_heads + kh + 1]
            query_col = columns[:, kh : kh + 1]
            faded = state[row, head] * row_dec[head : head + 1, :]
            predicted = jnp.sum(faded * key_col, axis=0, keepdims=True)
            correction = row_beta[head : head + 1, :] * (row_vals[head : head + 1, :] - predicted)
            updated = faded + key_col * correction
            state[row, head] = updated
            read_rows[row, head : head + 1, :] = jnp.sum(updated * query_col, axis=0, keepdims=True)
        pltpu.make_async_copy(state.at[row], state_out_hbm.at[row], out_sem.at[row]).start()
        return carry

    lax.fori_loop(0, own_rows, step, 0)

    out_gate = silu(collect(copies_c, smc, rmc) * scale)
    for head in range(heads):
        reading = read_rows[:, head, :]
        mean = jnp.mean(reading * reading, axis=1, keepdims=True)
        normed = reading * lax.rsqrt(mean + EPS) * head_gain_ref[...]
        cols = slice(head * size, (head + 1) * size)
        nrm[kv, :, cols] = (normed * out_gate[:, cols]).astype(BF16)
    copies = gather(8, "kv", kv, n_kv, nrm.at[kv], nrm)
    loads[7].wait()
    for copy in copies:
        copy.wait_recv()
    branch = exchange(9, dot(flat(nrm), wout[...]), parm)
    after_mixer = (after_first + branch).astype(BF16).astype(F32)

    final = half_ffn(
        10, after_mixer, gain_second_ref, 8, gate2, up2, down2, (s2a, r2a, s2b, r2b), hid2, par2
    )
    row_id = lax.broadcasted_iota(jnp.int32, (depth, piece), 0)
    col_id = lax.broadcasted_iota(jnp.int32, (depth, piece), 1)
    pick = jnp.where(row_id == col_id + tp * piece, 1.0, 0.0).astype(F32).astype(BF16)
    res_out_ref[...] = dot(final, pick).astype(BF16)

    for copy in pending:
        copy.wait_send()

    def drain(row, carry):
        pltpu.make_async_copy(state.at[row], state_out_hbm.at[row], out_sem.at[row]).wait()
        return carry

    lax.fori_loop(0, own_rows, drain, 0)


def place_heads(rows, first, lane_start, count):
    row = lax.broadcasted_iota(jnp.int32, (rows, LANES), 0)
    col = lax.broadcasted_iota(jnp.int32, (rows, LANES), 1)
    inside = (col >= lane_start) & (col < lane_start + count)
    hit = inside & (row == col - lane_start + first)
    return jnp.where(hit, 1.0, 0.0).astype(F32).astype(BF16)


def body(
    n_kv,
    n_tp,
    residual_in,
    delta_state,
    norm_gain_first,
    gate_first,
    up_first,
    down_first,
    norm_gain_mixer,
    query_weight,
    key_weight,
    value_weight,
    output_gate_weight,
    beta_weight,
    decay_weight,
    decay_rate,
    decay_bias,
    head_gain,
    out_weight,
    norm_gain_second,
    gate_second,
    up_second,
    down_second,
):
    batch, piece = residual_in.shape
    depth, hidden = gate_first.shape
    own_rows, heads, size, _ = delta_state.shape
    key_cols = query_weight.shape[1]
    val_cols = value_weight.shape[1]
    key_heads = key_cols // size
    hp = pad_lanes(hidden)

    def like(x):
        return pltpu.VMEM(x.shape, x.dtype)

    def slots(cols):
        return pltpu.VMEM((n_kv, own_rows, cols), BF16)

    def row_buf(count):
        return pltpu.VMEM((own_rows, count, size), F32)

    tp_slots = pltpu.VMEM((n_tp, batch, depth), BF16)
    ffn_bufs = [slots(hp)] * 2 + [slots(hp + LANES)] * 2 + [slots(hidden), tp_slots]
    mixer_bufs = (
        [slots(2 * key_cols + LANES)] * 2
        + [slots(val_cols)] * 4
        + [slots(heads * size), tp_slots]
    )
    big = (
        gate_first,
        up_first,
        down_first,
        query_weight,
        key_weight,
        value_weight,
        output_gate_weight,
        out_weight,
        gate_second,
        up_second,
        down_second,
    )
    small = (
        residual_in,
        norm_gain_first[None, :],
        norm_gain_mixer[None, :],
        norm_gain_second[None, :],
        beta_weight,
        decay_weight,
        decay_rate[None, :],
        decay_bias[None, :],
        head_gain[None, :],
    )
    vmem = pl.BlockSpec(memory_space=pltpu.VMEM)
    hbm = pl.BlockSpec(memory_space=pl.ANY)
    most = max(n_kv, n_tp)
    return pl.pallas_call(
        functools.partial(kernel, n_kv, n_tp),
        out_shape=(
            jax.ShapeDtypeStruct(residual_in.shape, BF16),
            jax.ShapeDtypeStruct(delta_state.shape, F32),
        ),
        in_specs=[vmem] * len(small) + [hbm] * (1 + len(big)),
        out_specs=(vmem, hbm),
        scratch_shapes=[like(x) for x in big]
        + [like(delta_state), pltpu.VMEM((n_tp, batch, piece), BF16)]
        + ffn_bufs
        + mixer_bufs
        + ffn_bufs
        + [row_buf(2 * key_heads), row_buf(heads), row_buf(heads), row_buf(heads), row_buf(heads)]
        + [
            pltpu.SemaphoreType.DMA((len(big),)),
            pltpu.SemaphoreType.DMA((own_rows,)),
            pltpu.SemaphoreType.DMA((own_rows,)),
            pltpu.SemaphoreType.DMA((14, most)),
            pltpu.SemaphoreType.DMA((14, most)),
        ],
        compiler_params=pltpu.CompilerParams(
            collective_id=0, has_side_effects=True, vmem_limit_bytes=60 * 1024 * 1024
        ),
        name="layer",
    )(*small, delta_state, *big)


def solution(mesh):
    placed = (
        P(None, ("kv", "tp")),
        P("kv", "tp", None, None),
        P("kv"),
        P("kv", "tp"),
        P("kv", "tp"),
        P("tp", "kv"),
        P("kv"),
        P("kv", "tp"),
        P("kv", "tp"),
        P("kv", "tp"),
        P("kv", "tp"),
        P("kv", None),
        P("kv", None),
        P("tp"),
        P("tp"),
        P(),
        P("tp", "kv"),
        P("kv"),
        P("kv", "tp"),
        P("kv", "tp"),
        P("tp", "kv"),
    )
    return jax.shard_map(
        functools.partial(body, mesh.shape["kv"], mesh.shape["tp"]),
        mesh=mesh,
        in_specs=placed,
        out_specs=(P(None, ("kv", "tp")), P("kv", "tp", None, None)),
        check_vma=False,
    )
```

```python
import functools

import jax
import jax.numpy as jnp
from jax import lax
from jax.experimental import pallas as pl
from jax.experimental.pallas import tpu as pltpu
from jax.sharding import PartitionSpec as P

EPS = 1e-06
LANES = 128
BF16 = jnp.bfloat16
F32 = jnp.float32


def pad_lanes(size):
    return -(-size // LANES) * LANES


def silu(v):
    return v / (1.0 + jnp.exp(-v))


def dot(a, b):
    return jnp.dot(a, b, preferred_element_type=F32)


def dot_first(a, b):
    return lax.dot_general(a, b, (((0,), (0,)), ((), ())), preferred_element_type=F32)


def inner_size(count):
    size = 1
    while size * size * 4 <= count and count % (size * 2) == 0:
        size *= 2
    return size


def ffn_chunks(cols):
    units = -(-cols // LANES)
    cut = -(-units // 2) * LANES
    return ((0, cut), (cut, cols - cut)) if cut < cols else ((0, cols),)


def place(rows, cols, shift):
    row = lax.broadcasted_iota(jnp.int32, (rows, cols), 0)
    col = lax.broadcasted_iota(jnp.int32, (rows, cols), 1)
    return jnp.where(col == row + shift, 1.0, 0.0).astype(F32).astype(BF16)


def kernel(
    n_kv,
    n_tp,
    res_ref,
    gain_first_ref,
    gain_mixer_ref,
    gain_second_ref,
    beta_ref,
    decay_ref,
    rate_ref,
    bias_ref,
    head_gain_ref,
    state_hbm,
    gate1_hbm,
    up1_hbm,
    down1_hbm,
    wq_hbm,
    wk_hbm,
    wv_hbm,
    wo_hbm,
    out_hbm,
    gate2_hbm,
    up2_hbm,
    down2_hbm,
    res_out_ref,
    state_out_hbm,
    gate1,
    up1,
    down1,
    wq,
    wk,
    wv,
    wo,
    wout,
    gate2,
    up2,
    down2,
    state,
    res_all,
    *rest,
):
    n_in = inner_size(n_kv)
    n_out = n_kv // n_in
    chunks = len(ffn_chunks(gate1.shape[1]))
    rest = list(rest)

    def take(count):
        taken = rest[:count]
        del rest[:count]
        return taken

    ffn1 = take(5 * chunks)
    ffn2 = take(5 * chunks)
    mixer = take(12)
    par1, parm, fin_send, fin_recv, nrm = take(5)
    (
        qk_rows,
        val_rows,
        beta_rows,
        dec_rows,
        read_rows,
        w_sem,
        in_sem,
        out_sem,
        send_sem,
        recv_sem,
    ) = rest
    kv = lax.axis_index("kv")
    tp = lax.axis_index("tp")
    outer, inner = kv // n_in, lax.rem(kv, n_in)
    batch, piece = res_ref.shape
    depth = gate1.shape[0]
    width = depth * n_kv
    own_rows = batch // n_kv
    heads = state.shape[1]
    size = state.shape[2]
    key_cols = wq.shape[1]
    key_heads = key_cols // size
    repeat = heads // key_heads
    val_cols = wv.shape[1]

    weight_pairs = (
        (gate1_hbm, gate1),
        (up1_hbm, up1),
        (down1_hbm, down1),
        (wq_hbm, wq),
        (wk_hbm, wk),
        (wv_hbm, wv),
        (wo_hbm, wo),
        (out_hbm, wout),
        (gate2_hbm, gate2),
        (up2_hbm, up2),
        (down2_hbm, down2),
    )
    loads = [
        pltpu.make_async_copy(src, dst, w_sem.at[i]) for i, (src, dst) in enumerate(weight_pairs)
    ]
    for load in loads[:7]:
        load.start()

    barrier = pltpu.get_barrier_semaphore()
    for off in range(1, n_tp):
        pl.semaphore_signal(
            barrier,
            inc=1,
            device_id={"tp": lax.rem(tp + off, n_tp)},
            device_id_type=pl.DeviceIdType.MESH,
        )
    for off in range(1, n_kv):
        pl.semaphore_signal(
            barrier,
            inc=1,
            device_id={"kv": lax.rem(kv + off, n_kv)},
            device_id_type=pl.DeviceIdType.MESH,
        )
    pl.semaphore_wait(barrier, n_tp - 1 + n_kv - 1)

    pending = []

    def send(event, off, src, dst, axis, peer):
        copy = pltpu.make_async_remote_copy(
            src_ref=src,
            dst_ref=dst,
            send_sem=send_sem.at[event, off],
            recv_sem=recv_sem.at[event, off],
            device_id={axis: peer},
            device_id_type=pl.DeviceIdType.MESH,
        )
        copy.start()
        pending.append(copy)
        return copy

    def gather(event, axis, me, count, own, slots):
        return [
            send(event, off, own, slots.at[me], axis, lax.rem(me + off, count))
            for off in range(1, count)
        ]

    def put(ref, offset, value):
        cols = value.shape[1]
        parts = value.reshape(n_out, n_in, own_rows, cols).astype(BF16)
        for side in range(n_in):
            ref[side, :, :, offset : offset + cols] = parts[:, side]

    def scatter_inner(event, bufs):
        copies = []
        for off in range(1, n_in):
            side = lax.rem(inner + off, n_in)
            peer = outer * n_in + side
            copies.append(send(event, off, bufs[0].at[side], bufs[1].at[inner], "kv", peer))
        return copies

    def scatter_outer(event, copies, bufs):
        mine, theirs, send_buf, recv_buf = bufs[:4]
        total = mine[inner].astype(F32)
        for off in range(1, n_in):
            copies[off - 1].wait_recv()
            total = total + theirs[lax.rem(inner + n_in - off, n_in)].astype(F32)
        send_buf[...] = total.astype(BF16)
        sent = []
        for off in range(1, n_out):
            line = lax.rem(outer + off, n_out)
            peer = line * n_in + inner
            sent.append(send(event, off, send_buf.at[line], recv_buf.at[outer], "kv", peer))
        return sent

    def collect(copies, bufs):
        send_buf, recv_buf = bufs[2:4]
        total = send_buf[outer].astype(F32)
        for off in range(1, n_out):
            copies[off - 1].wait_recv()
            total = total + recv_buf[lax.rem(outer + n_out - off, n_out)].astype(F32)
        return total

    def spread(event, slots):
        line = []
        for off in range(1, n_out):
            peer = lax.rem(outer + off, n_out) * n_in + inner
            line.append(send(event, off, slots.at[kv], slots.at[kv], "kv", peer))
        near = []
        for off in range(1, n_in):
            peer = outer * n_in + lax.rem(inner + off, n_in)
            near.append(send(event + 1, off, slots.at[kv], slots.at[kv], "kv", peer))
        return line, near

    def relay(event, line, slots):
        passed = []
        for off in range(1, n_out):
            line[off - 1].wait_recv()
            slot = lax.rem(outer + n_out - off, n_out) * n_in + inner
            for side in range(1, n_in):
                peer = outer * n_in + lax.rem(inner + side, n_in)
                index = (off - 1) * (n_in - 1) + side - 1
                passed.append(send(event, index, slots.at[slot], slots.at[slot], "kv", peer))
        return passed

    def square_lanes(residual):
        squares = jnp.sum(residual * residual, axis=1, keepdims=True)
        high = squares.astype(BF16).astype(F32)
        lane = lax.broadcasted_iota(jnp.int32, (batch, LANES), 1)
        return jnp.where(lane == 64, high, jnp.where(lane == 65, squares - high, 0.0))

    def row_scale(extra):
        squares = extra[:, 64:65] + extra[:, 65:66]
        return lax.rsqrt(squares / width + EPS)

    def flat(slots):
        both = slots[...].astype(F32)
        return both.reshape(batch, both.shape[2]).astype(BF16)

    def exchange(event, value, slots):
        slots[tp] = value.astype(BF16)
        copies = gather(event, "tp", tp, n_tp, slots.at[tp], slots)
        for copy in copies:
            copy.wait_recv()
        total = slots[0].astype(F32)
        for other in range(1, n_tp):
            total = total + slots[other].astype(F32)
        return total

    def pick(peer):
        row = lax.broadcasted_iota(jnp.int32, (depth, piece), 0)
        col = lax.broadcasted_iota(jnp.int32, (depth, piece), 1)
        return jnp.where(row == col + peer * piece, 1.0, 0.0).astype(F32).astype(BF16)

    def half_ffn(event, residual, gain_ref, first, w_gate, w_up, w_down, bufs):
        spans = ffn_chunks(w_gate.shape[1])
        scaled = (residual * gain_ref[...]).astype(BF16)
        near, line, going = [], [], []
        for i, (start, cols) in enumerate(spans):
            own = bufs[5 * i : 5 * i + 5]
            step = pad_lanes(cols)
            if i == 0:
                loads[first].wait()
            put(own[0], 0, dot(scaled, w_gate[:, start : start + cols]))
            if i == 0:
                loads[first + 1].wait()
            put(own[0], step, dot(scaled, w_up[:, start : start + cols]))
            if i == 0:
                put(own[0], 2 * step, square_lanes(residual))
            near.append(scatter_inner(event + 5 * i, own))
        for i in range(len(spans)):
            line.append(scatter_outer(event + 5 * i + 1, near[i], bufs[5 * i : 5 * i + 5]))
        scale = None
        for i, (start, cols) in enumerate(spans):
            own = bufs[5 * i : 5 * i + 5]
            step = pad_lanes(cols)
            total = collect(line[i], own)
            if i == 0:
                scale = row_scale(total[:, 2 * step :])
            gate_act = total[:, :cols] * scale
            own[4][kv] = (silu(gate_act) * (total[:, step : step + cols] * scale)).astype(BF16)
            going.append(spread(event + 5 * i + 2, own[4]))
        passed = [
            relay(event + 5 * i + 4, going[i][0], bufs[5 * i + 4]) for i in range(len(spans))
        ]
        loads[first + 2].wait()
        product = None
        for i, (start, cols) in enumerate(spans):
            for copy in going[i][1] + passed[i]:
                copy.wait_recv()
            part = dot(flat(bufs[5 * i + 4]), w_down[start : start + cols, :])
            product = part if product is None else product + part
        return product

    copies = gather(0, "tp", tp, n_tp, res_ref, res_all)
    for load in loads[7:]:
        load.start()
    for row in range(own_rows):
        pltpu.make_async_copy(state_hbm.at[row], state.at[row], in_sem.at[row]).start()
    decay_exp = jnp.exp(rate_ref[...])
    extra_weight = (
        dot_first(beta_ref[...], place_heads(beta_ref.shape[0], tp * heads, 0, heads))
        + dot_first(decay_ref[...], place_heads(beta_ref.shape[0], tp * heads, heads, heads))
    ).astype(BF16)
    residual = dot(res_ref[...], place(piece, depth, tp * piece))
    for off in range(1, n_tp):
        copies[off - 1].wait_recv()
        source = lax.rem(tp + n_tp - off, n_tp)
        residual = residual + dot(res_all[source], place(piece, depth, source * piece))

    product = half_ffn(1, residual, gain_first_ref, 0, gate1, up1, down1, ffn1)
    e = 1 + 5 * chunks
    branch = exchange(e, product, par1)
    after_first = (residual + 0.5 * branch).astype(BF16).astype(F32)

    scaled = (after_first * gain_mixer_ref[...]).astype(BF16)
    bufs_a, bufs_b, bufs_c = mixer[:4], mixer[4:8], mixer[8:]
    loads[3].wait()
    put(bufs_a[0], 0, dot(scaled, wq[...]))
    loads[4].wait()
    put(bufs_a[0], key_cols, dot(scaled, wk[...]))
    put(bufs_a[0], 2 * key_cols, dot(scaled, extra_weight) + square_lanes(after_first))
    near_a = scatter_inner(e + 1, bufs_a)
    loads[5].wait()
    put(bufs_b[0], 0, dot(scaled, wv[...]))
    near_b = scatter_inner(e + 2, bufs_b)
    loads[6].wait()
    put(bufs_c[0], 0, dot(scaled, wo[...]))
    near_c = scatter_inner(e + 3, bufs_c)
    line_a = scatter_outer(e + 4, near_a, bufs_a)
    line_b = scatter_outer(e + 5, near_b, bufs_b)
    line_c = scatter_outer(e + 6, near_c, bufs_c)

    keys_sum = collect(line_a, bufs_a)
    extra = keys_sum[:, 2 * key_cols :]
    scale = row_scale(extra)
    for head in range(key_heads):
        for slot, start, factor in (
            (head, head * size, size ** (-0.5)),
            (key_heads + head, key_cols + head * size, 1.0),
        ):
            act = silu(keys_sum[:, start : start + size] * scale)
            unit = act * lax.rsqrt(jnp.sum(act * act, axis=1, keepdims=True) + EPS)
            qk_rows[:, slot, :] = unit * factor
    gates = extra * scale
    beta_pre = gates[:, :heads]
    decay_pre = gates[:, heads : 2 * heads] + bias_ref[...]
    beta_gate = 1.0 / (1.0 + jnp.exp(-beta_pre))
    softplus = jnp.maximum(decay_pre, 0.0) + jnp.log1p(jnp.exp(-jnp.abs(decay_pre)))
    decay_gate = jnp.exp(-decay_exp * softplus)
    for head in range(heads):
        beta_rows[:, head, :] = jnp.broadcast_to(beta_gate[:, head : head + 1], (own_rows, size))
        dec_rows[:, head, :] = jnp.broadcast_to(decay_gate[:, head : head + 1], (own_rows, size))
    values = silu(collect(line_b, bufs_b) * scale)
    for head in range(heads):
        val_rows[:, head, :] = values[:, head * size : (head + 1) * size]

    def step(row, carry):
        pltpu.make_async_copy(state_hbm.at[row], state.at[row], in_sem.at[row]).wait()
        columns = qk_rows[row].T
        row_vals, row_beta, row_dec = val_rows[row], beta_rows[row], dec_rows[row]
        for head in range(heads):
            kh = head // repeat
            key_col = columns[:, key_heads + kh : key_heads + kh + 1]
            query_col = columns[:, kh : kh + 1]
            faded = state[row, head] * row_dec[head : head + 1, :]
            predicted = jnp.sum(faded * key_col, axis=0, keepdims=True)
            correction = row_beta[head : head + 1, :] * (row_vals[head : head + 1, :] - predicted)
            updated = faded + key_col * correction
            state[row, head] = updated
            read_rows[row, head : head + 1, :] = jnp.sum(updated * query_col, axis=0, keepdims=True)
        pltpu.make_async_copy(state.at[row], state_out_hbm.at[row], out_sem.at[row]).start()
        return carry

    lax.fori_loop(0, own_rows, step, 0)

    out_gate = silu(collect(line_c, bufs_c) * scale)
    for head in range(heads):
        reading = read_rows[:, head, :]
        mean = jnp.mean(reading * reading, axis=1, keepdims=True)
        normed = reading * lax.rsqrt(mean + EPS) * head_gain_ref[...]
        cols = slice(head * size, (head + 1) * size)
        nrm[kv, :, cols] = (normed * out_gate[:, cols]).astype(BF16)
    copies = gather(e + 7, "kv", kv, n_kv, nrm.at[kv], nrm)
    loads[7].wait()
    for copy in copies:
        copy.wait_recv()
    branch = exchange(e + 8, dot(flat(nrm), wout[...]), parm)
    after_mixer = (after_first + branch).astype(BF16).astype(F32)

    product = half_ffn(e + 9, after_mixer, gain_second_ref, 8, gate2, up2, down2, ffn2)
    product = product.astype(BF16)
    copies = []
    for off in range(1, n_tp):
        peer = lax.rem(tp + off, n_tp)
        fin_send[off] = dot(product, pick(peer)).astype(BF16)
        event = e + 9 + 5 * chunks
        copies.append(send(event, off, fin_send.at[off], fin_recv.at[off], "tp", peer))
    mine = pick(tp)
    own_cols = dot(after_mixer.astype(BF16), mine)
    branch = dot(product, mine)
    for off in range(1, n_tp):
        copies[off - 1].wait_recv()
        branch = branch + fin_recv[off].astype(F32)
    res_out_ref[...] = (own_cols + 0.5 * branch).astype(BF16)

    for copy in pending:
        copy.wait_send()

    def drain(row, carry):
        pltpu.make_async_copy(state.at[row], state_out_hbm.at[row], out_sem.at[row]).wait()
        return carry

    lax.fori_loop(0, own_rows, drain, 0)


def place_heads(rows, first, lane_start, count):
    row = lax.broadcasted_iota(jnp.int32, (rows, LANES), 0)
    col = lax.broadcasted_iota(jnp.int32, (rows, LANES), 1)
    inside = (col >= lane_start) & (col < lane_start + count)
    hit = inside & (row == col - lane_start + first)
    return jnp.where(hit, 1.0, 0.0).astype(F32).astype(BF16)


def body(
    n_kv,
    n_tp,
    residual_in,
    delta_state,
    norm_gain_first,
    gate_first,
    up_first,
    down_first,
    norm_gain_mixer,
    query_weight,
    key_weight,
    value_weight,
    output_gate_weight,
    beta_weight,
    decay_weight,
    decay_rate,
    decay_bias,
    head_gain,
    out_weight,
    norm_gain_second,
    gate_second,
    up_second,
    down_second,
):
    batch, piece = residual_in.shape
    depth, hidden = gate_first.shape
    own_rows, heads, size, _ = delta_state.shape
    key_cols = query_weight.shape[1]
    val_cols = value_weight.shape[1]
    key_heads = key_cols // size
    n_in = inner_size(n_kv)
    n_out = n_kv // n_in
    def like(x):
        return pltpu.VMEM(x.shape, x.dtype)

    def slots(cols):
        return pltpu.VMEM((n_kv, own_rows, cols), BF16)

    def two_stage(cols):
        near = pltpu.VMEM((n_in, n_out, own_rows, cols), BF16)
        line = pltpu.VMEM((n_out, own_rows, cols), BF16)
        return [near, near, line, line]

    def row_buf(count):
        return pltpu.VMEM((own_rows, count, size), F32)

    tp_slots = pltpu.VMEM((n_tp, batch, depth), BF16)
    ffn_bufs = []
    for i, (_, cols) in enumerate(ffn_chunks(hidden)):
        extra = LANES if i == 0 else 0
        ffn_bufs += two_stage(2 * pad_lanes(cols) + extra) + [slots(cols)]
    mixer_bufs = (
        two_stage(2 * key_cols + LANES) + two_stage(val_cols) + two_stage(val_cols)
    )
    final_buf = pltpu.VMEM((n_tp, batch, piece), BF16)
    last_bufs = [tp_slots, tp_slots, final_buf, final_buf, slots(heads * size)]
    events = 11 + 2 * len(ffn_bufs)
    big = (
        gate_first,
        up_first,
        down_first,
        query_weight,
        key_weight,
        value_weight,
        output_gate_weight,
        out_weight,
        gate_second,
        up_second,
        down_second,
    )
    small = (
        residual_in,
        norm_gain_first[None, :],
        norm_gain_mixer[None, :],
        norm_gain_second[None, :],
        beta_weight.T,
        decay_weight.T,
        decay_rate[None, :],
        decay_bias[None, :],
        head_gain[None, :],
    )
    vmem = pl.BlockSpec(memory_space=pltpu.VMEM)
    hbm = pl.BlockSpec(memory_space=pl.ANY)
    most = max(n_kv, n_tp)
    return pl.pallas_call(
        functools.partial(kernel, n_kv, n_tp),
        out_shape=(
            jax.ShapeDtypeStruct(residual_in.shape, BF16),
            jax.ShapeDtypeStruct(delta_state.shape, F32),
        ),
        in_specs=[vmem] * len(small) + [hbm] * (1 + len(big)),
        out_specs=(vmem, hbm),
        scratch_shapes=[like(x) for x in big]
        + [like(delta_state), pltpu.VMEM((n_tp, batch, piece), BF16)]
        + ffn_bufs
        + ffn_bufs
        + mixer_bufs
        + last_bufs
        + [row_buf(2 * key_heads), row_buf(heads), row_buf(heads), row_buf(heads), row_buf(heads)]
        + [
            pltpu.SemaphoreType.DMA((len(big),)),
            pltpu.SemaphoreType.DMA((own_rows,)),
            pltpu.SemaphoreType.DMA((own_rows,)),
            pltpu.SemaphoreType.DMA((events, most)),
            pltpu.SemaphoreType.DMA((events, most)),
        ],
        compiler_params=pltpu.CompilerParams(
            collective_id=0, has_side_effects=True, vmem_limit_bytes=60 * 1024 * 1024
        ),
        name="layer",
    )(*small, delta_state, *big)


def solution(mesh):
    placed = (
        P(None, ("kv", "tp")),
        P("kv", "tp", None, None),
        P("kv"),
        P("kv", "tp"),
        P("kv", "tp"),
        P("tp", "kv"),
        P("kv"),
        P("kv", "tp"),
        P("kv", "tp"),
        P("kv", "tp"),
        P("kv", "tp"),
        P("kv", None),
        P("kv", None),
        P("tp"),
        P("tp"),
        P(),
        P("tp", "kv"),
        P("kv"),
        P("kv", "tp"),
        P("kv", "tp"),
        P("tp", "kv"),
    )
    return jax.shard_map(
        functools.partial(body, mesh.shape["kv"], mesh.shape["tp"]),
        mesh=mesh,
        in_specs=placed,
        out_specs=(P(None, ("kv", "tp")), P("kv", "tp", None, None)),
        check_vma=False,
    )
```

```python
import functools

import jax
import jax.numpy as jnp
from jax import lax
from jax.experimental import pallas as pl
from jax.experimental.pallas import tpu as pltpu
from jax.sharding import PartitionSpec as P

EPS = 1e-06
LANES = 128
BF16 = jnp.bfloat16
F32 = jnp.float32


def pad_lanes(size):
    return -(-size // LANES) * LANES


def silu(v):
    return v / (1.0 + jnp.exp(-v))


def dot(a, b):
    return jnp.dot(a, b, preferred_element_type=F32)


def dot_first(a, b):
    return lax.dot_general(a, b, (((0,), (0,)), ((), ())), preferred_element_type=F32)


def place(rows, cols, shift):
    row = lax.broadcasted_iota(jnp.int32, (rows, cols), 0)
    col = lax.broadcasted_iota(jnp.int32, (rows, cols), 1)
    return jnp.where(col == row + shift, 1.0, 0.0).astype(F32).astype(BF16)


def kernel(
    n_kv,
    n_tp,
    res_ref,
    gain_first_ref,
    gain_mixer_ref,
    gain_second_ref,
    beta_ref,
    decay_ref,
    rate_ref,
    bias_ref,
    head_gain_ref,
    state_hbm,
    gate1_hbm,
    up1_hbm,
    down1_hbm,
    wq_hbm,
    wk_hbm,
    wv_hbm,
    wo_hbm,
    out_hbm,
    gate2_hbm,
    up2_hbm,
    down2_hbm,
    res_out_ref,
    state_out_hbm,
    gate1,
    up1,
    down1,
    wq,
    wk,
    wv,
    wo,
    wout,
    gate2,
    up2,
    down2,
    state,
    res_all,
    s1a,
    r1a,
    s1b,
    r1b,
    hid1,
    par1,
    sma,
    rma,
    smb,
    rmb,
    smc,
    rmc,
    nrm,
    parm,
    s2a,
    r2a,
    s2b,
    r2b,
    hid2,
    fin_send,
    fin_recv,
    qk_rows,
    val_rows,
    beta_rows,
    dec_rows,
    read_rows,
    w_sem,
    in_sem,
    out_sem,
    send_sem,
    recv_sem,
):
    kv = lax.axis_index("kv")
    tp = lax.axis_index("tp")
    batch, piece = res_ref.shape
    depth = gate1.shape[0]
    width = depth * n_kv
    own_rows = batch // n_kv
    heads = state.shape[1]
    size = state.shape[2]
    key_cols = wq.shape[1]
    key_heads = key_cols // size
    repeat = heads // key_heads
    val_cols = wv.shape[1]

    weight_pairs = (
        (gate1_hbm, gate1),
        (up1_hbm, up1),
        (down1_hbm, down1),
        (wq_hbm, wq),
        (wk_hbm, wk),
        (wv_hbm, wv),
        (wo_hbm, wo),
        (out_hbm, wout),
        (gate2_hbm, gate2),
        (up2_hbm, up2),
        (down2_hbm, down2),
    )
    loads = [
        pltpu.make_async_copy(src, dst, w_sem.at[i]) for i, (src, dst) in enumerate(weight_pairs)
    ]
    for load in loads[:7]:
        load.start()

    barrier = pltpu.get_barrier_semaphore()
    for off in range(1, n_tp):
        pl.semaphore_signal(
            barrier,
            inc=1,
            device_id={"tp": lax.rem(tp + off, n_tp)},
            device_id_type=pl.DeviceIdType.MESH,
        )
    for off in range(1, n_kv):
        pl.semaphore_signal(
            barrier,
            inc=1,
            device_id={"kv": lax.rem(kv + off, n_kv)},
            device_id_type=pl.DeviceIdType.MESH,
        )
    pl.semaphore_wait(barrier, n_tp - 1 + n_kv - 1)

    pending = []

    def send(event, off, src, dst, axis, peer):
        copy = pltpu.make_async_remote_copy(
            src_ref=src,
            dst_ref=dst,
            send_sem=send_sem.at[event, off],
            recv_sem=recv_sem.at[event, off],
            device_id={axis: peer},
            device_id_type=pl.DeviceIdType.MESH,
        )
        copy.start()
        pending.append(copy)
        return copy

    def gather(event, axis, me, count, own, slots):
        return [
            send(event, off, own, slots.at[me], axis, lax.rem(me + off, count))
            for off in range(1, count)
        ]

    def scatter(event, sends, receives):
        copies = []
        for off in range(1, n_kv):
            peer = lax.rem(kv + off, n_kv)
            copies.append(send(event, off, sends.at[peer], receives.at[kv], "kv", peer))
        return copies

    def collect(copies, sends, receives):
        total = sends[kv].astype(F32)
        for off in range(1, n_kv):
            copies[off - 1].wait_recv()
            source = lax.rem(kv + n_kv - off, n_kv)
            total = total + receives[source].astype(F32)
        return total

    def put(ref, offset, value):
        cols = value.shape[1]
        ref[:, :, offset : offset + cols] = value.reshape(n_kv, own_rows, cols).astype(BF16)

    def square_lanes(residual):
        squares = jnp.sum(residual * residual, axis=1, keepdims=True)
        high = squares.astype(BF16).astype(F32)
        lane = lax.broadcasted_iota(jnp.int32, (batch, LANES), 1)
        return jnp.where(lane == 64, high, jnp.where(lane == 65, squares - high, 0.0))

    def row_scale(extra):
        squares = extra[:, 64:65] + extra[:, 65:66]
        return lax.rsqrt(squares / width + EPS)

    def flat(slots):
        both = slots[...].astype(F32)
        return both.reshape(batch, both.shape[2]).astype(BF16)

    def exchange(event, value, slots):
        slots[tp] = value.astype(BF16)
        copies = gather(event, "tp", tp, n_tp, slots.at[tp], slots)
        for copy in copies:
            copy.wait_recv()
        total = slots[0].astype(F32)
        for other in range(1, n_tp):
            total = total + slots[other].astype(F32)
        return total

    def half_ffn(event, residual, gain_ref, first, w_gate, w_up, w_down, bufs, hid):
        send_a, recv_a, send_b, recv_b = bufs
        hidden_cols = w_gate.shape[1]
        up_end = pad_lanes(hidden_cols)
        scaled = (residual * gain_ref[...]).astype(BF16)
        loads[first].wait()
        put(send_a, 0, dot(scaled, w_gate[...]))
        copies_a = scatter(event, send_a, recv_a)
        loads[first + 1].wait()
        put(send_b, 0, dot(scaled, w_up[...]))
        put(send_b, up_end, square_lanes(residual))
        copies_b = scatter(event + 1, send_b, recv_b)
        gate_sum = collect(copies_a, send_a, recv_a)[:, :hidden_cols]
        rest = collect(copies_b, send_b, recv_b)
        scale = row_scale(rest[:, up_end:])
        hidden = (silu(gate_sum * scale) * (rest[:, :hidden_cols] * scale)).astype(BF16)
        hid[kv] = hidden
        copies = gather(event + 2, "kv", kv, n_kv, hid.at[kv], hid)
        loads[first + 2].wait()
        for copy in copies:
            copy.wait_recv()
        return dot(flat(hid), w_down[...])

    copies = gather(0, "tp", tp, n_tp, res_ref, res_all)
    for load in loads[7:]:
        load.start()
    for row in range(own_rows):
        pltpu.make_async_copy(state_hbm.at[row], state.at[row], in_sem.at[row]).start()
    decay_exp = jnp.exp(rate_ref[...])
    extra_weight = (
        dot_first(beta_ref[...], place_heads(beta_ref.shape[0], tp * heads, 0, heads))
        + dot_first(decay_ref[...], place_heads(beta_ref.shape[0], tp * heads, heads, heads))
    ).astype(BF16)
    residual = dot(res_ref[...], place(piece, depth, tp * piece))
    for off in range(1, n_tp):
        copies[off - 1].wait_recv()
        source = lax.rem(tp + n_tp - off, n_tp)
        residual = residual + dot(res_all[source], place(piece, depth, source * piece))

    product = half_ffn(
        1, residual, gain_first_ref, 0, gate1, up1, down1, (s1a, r1a, s1b, r1b), hid1
    )
    branch = exchange(4, product, par1)
    after_first = (residual + 0.5 * branch).astype(BF16).astype(F32)

    scaled = (after_first * gain_mixer_ref[...]).astype(BF16)
    loads[3].wait()
    put(sma, 0, dot(scaled, wq[...]))
    loads[4].wait()
    put(sma, key_cols, dot(scaled, wk[...]))
    put(sma, 2 * key_cols, dot(scaled, extra_weight) + square_lanes(after_first))
    copies_a = scatter(5, sma, rma)
    loads[5].wait()
    put(smb, 0, dot(scaled, wv[...]))
    copies_b = scatter(6, smb, rmb)
    loads[6].wait()
    put(smc, 0, dot(scaled, wo[...]))
    copies_c = scatter(7, smc, rmc)

    keys_sum = collect(copies_a, sma, rma)
    extra = keys_sum[:, 2 * key_cols :]
    scale = row_scale(extra)
    for head in range(key_heads):
        for slot, start, factor in (
            (head, head * size, size ** (-0.5)),
            (key_heads + head, key_cols + head * size, 1.0),
        ):
            act = silu(keys_sum[:, start : start + size] * scale)
            unit = act * lax.rsqrt(jnp.sum(act * act, axis=1, keepdims=True) + EPS)
            qk_rows[:, slot, :] = unit * factor
    gates = extra * scale
    beta_pre = gates[:, :heads]
    decay_pre = gates[:, heads : 2 * heads] + bias_ref[...]
    beta_gate = 1.0 / (1.0 + jnp.exp(-beta_pre))
    softplus = jnp.maximum(decay_pre, 0.0) + jnp.log1p(jnp.exp(-jnp.abs(decay_pre)))
    decay_gate = jnp.exp(-decay_exp * softplus)
    for head in range(heads):
        beta_rows[:, head, :] = jnp.broadcast_to(beta_gate[:, head : head + 1], (own_rows, size))
        dec_rows[:, head, :] = jnp.broadcast_to(decay_gate[:, head : head + 1], (own_rows, size))
    values = silu(collect(copies_b, smb, rmb) * scale)
    for head in range(heads):
        val_rows[:, head, :] = values[:, head * size : (head + 1) * size]

    def step(row, carry):
        pltpu.make_async_copy(state_hbm.at[row], state.at[row], in_sem.at[row]).wait()
        columns = qk_rows[row].T
        row_vals, row_beta, row_dec = val_rows[row], beta_rows[row], dec_rows[row]
        for head in range(heads):
            kh = head // repeat
            key_col = columns[:, key_heads + kh : key_heads + kh + 1]
            query_col = columns[:, kh : kh + 1]
            faded = state[row, head] * row_dec[head : head + 1, :]
            predicted = jnp.sum(faded * key_col, axis=0, keepdims=True)
            correction = row_beta[head : head + 1, :] * (row_vals[head : head + 1, :] - predicted)
            updated = faded + key_col * correction
            state[row, head] = updated
            read_rows[row, head : head + 1, :] = jnp.sum(updated * query_col, axis=0, keepdims=True)
        pltpu.make_async_copy(state.at[row], state_out_hbm.at[row], out_sem.at[row]).start()
        return carry

    lax.fori_loop(0, own_rows, step, 0)

    out_gate = silu(collect(copies_c, smc, rmc) * scale)
    for head in range(heads):
        reading = read_rows[:, head, :]
        mean = jnp.mean(reading * reading, axis=1, keepdims=True)
        normed = reading * lax.rsqrt(mean + EPS) * head_gain_ref[...]
        cols = slice(head * size, (head + 1) * size)
        nrm[kv, :, cols] = (normed * out_gate[:, cols]).astype(BF16)
    copies = gather(8, "kv", kv, n_kv, nrm.at[kv], nrm)
    loads[7].wait()
    for copy in copies:
        copy.wait_recv()
    branch = exchange(9, dot(flat(nrm), wout[...]), parm)
    after_mixer = (after_first + branch).astype(BF16).astype(F32)

    product = half_ffn(
        10, after_mixer, gain_second_ref, 8, gate2, up2, down2, (s2a, r2a, s2b, r2b), hid2
    ).astype(BF16)
    copies = []
    for off in range(1, n_tp):
        peer = lax.rem(tp + off, n_tp)
        fin_send[off] = dot(product, place_back(depth, piece, peer)).astype(BF16)
        copies.append(send(13, off, fin_send.at[off], fin_recv.at[off], "tp", peer))
    mine = place_back(depth, piece, tp)
    own_cols = dot(after_mixer.astype(BF16), mine)
    branch = dot(product, mine)
    for off in range(1, n_tp):
        copies[off - 1].wait_recv()
        branch = branch + fin_recv[off].astype(F32)
    res_out_ref[...] = (own_cols + 0.5 * branch).astype(BF16)

    for copy in pending:
        copy.wait_send()

    def drain(row, carry):
        pltpu.make_async_copy(state.at[row], state_out_hbm.at[row], out_sem.at[row]).wait()
        return carry

    lax.fori_loop(0, own_rows, drain, 0)


def place_back(rows, cols, peer):
    row = lax.broadcasted_iota(jnp.int32, (rows, cols), 0)
    col = lax.broadcasted_iota(jnp.int32, (rows, cols), 1)
    return jnp.where(row == col + peer * cols, 1.0, 0.0).astype(F32).astype(BF16)


def place_heads(rows, first, lane_start, count):
    row = lax.broadcasted_iota(jnp.int32, (rows, LANES), 0)
    col = lax.broadcasted_iota(jnp.int32, (rows, LANES), 1)
    inside = (col >= lane_start) & (col < lane_start + count)
    hit = inside & (row == col - lane_start + first)
    return jnp.where(hit, 1.0, 0.0).astype(F32).astype(BF16)


def body(
    n_kv,
    n_tp,
    residual_in,
    delta_state,
    norm_gain_first,
    gate_first,
    up_first,
    down_first,
    norm_gain_mixer,
    query_weight,
    key_weight,
    value_weight,
    output_gate_weight,
    beta_weight,
    decay_weight,
    decay_rate,
    decay_bias,
    head_gain,
    out_weight,
    norm_gain_second,
    gate_second,
    up_second,
    down_second,
):
    batch, piece = residual_in.shape
    depth, hidden = gate_first.shape
    own_rows, heads, size, _ = delta_state.shape
    key_cols = query_weight.shape[1]
    val_cols = value_weight.shape[1]
    key_heads = key_cols // size
    hp = pad_lanes(hidden)

    def like(x):
        return pltpu.VMEM(x.shape, x.dtype)

    def slots(cols):
        return pltpu.VMEM((n_kv, own_rows, cols), BF16)

    def row_buf(count):
        return pltpu.VMEM((own_rows, count, size), F32)

    tp_slots = pltpu.VMEM((n_tp, batch, depth), BF16)
    ffn_bufs = [slots(hp)] * 2 + [slots(hp + LANES)] * 2 + [slots(hidden), tp_slots]
    mixer_bufs = (
        [slots(2 * key_cols + LANES)] * 2
        + [slots(val_cols)] * 4
        + [slots(heads * size), tp_slots]
    )
    big = (
        gate_first,
        up_first,
        down_first,
        query_weight,
        key_weight,
        value_weight,
        output_gate_weight,
        out_weight,
        gate_second,
        up_second,
        down_second,
    )
    small = (
        residual_in,
        norm_gain_first[None, :],
        norm_gain_mixer[None, :],
        norm_gain_second[None, :],
        beta_weight.T,
        decay_weight.T,
        decay_rate[None, :],
        decay_bias[None, :],
        head_gain[None, :],
    )
    vmem = pl.BlockSpec(memory_space=pltpu.VMEM)
    hbm = pl.BlockSpec(memory_space=pl.ANY)
    most = max(n_kv, n_tp)
    return pl.pallas_call(
        functools.partial(kernel, n_kv, n_tp),
        out_shape=(
            jax.ShapeDtypeStruct(residual_in.shape, BF16),
            jax.ShapeDtypeStruct(delta_state.shape, F32),
        ),
        in_specs=[vmem] * len(small) + [hbm] * (1 + len(big)),
        out_specs=(vmem, hbm),
        scratch_shapes=[like(x) for x in big]
        + [like(delta_state), pltpu.VMEM((n_tp, batch, piece), BF16)]
        + ffn_bufs
        + mixer_bufs
        + ffn_bufs[:-1]
        + [pltpu.VMEM((n_tp, batch, piece), BF16)] * 2
        + [row_buf(2 * key_heads), row_buf(heads), row_buf(heads), row_buf(heads), row_buf(heads)]
        + [
            pltpu.SemaphoreType.DMA((len(big),)),
            pltpu.SemaphoreType.DMA((own_rows,)),
            pltpu.SemaphoreType.DMA((own_rows,)),
            pltpu.SemaphoreType.DMA((14, most)),
            pltpu.SemaphoreType.DMA((14, most)),
        ],
        compiler_params=pltpu.CompilerParams(
            collective_id=0, has_side_effects=True, vmem_limit_bytes=60 * 1024 * 1024
        ),
        name="layer",
    )(*small, delta_state, *big)


def solution(mesh):
    placed = (
        P(None, ("kv", "tp")),
        P("kv", "tp", None, None),
        P("kv"),
        P("kv", "tp"),
        P("kv", "tp"),
        P("tp", "kv"),
        P("kv"),
        P("kv", "tp"),
        P("kv", "tp"),
        P("kv", "tp"),
        P("kv", "tp"),
        P("kv", None),
        P("kv", None),
        P("tp"),
        P("tp"),
        P(),
        P("tp", "kv"),
        P("kv"),
        P("kv", "tp"),
        P("kv", "tp"),
        P("tp", "kv"),
    )
    return jax.shard_map(
        functools.partial(body, mesh.shape["kv"], mesh.shape["tp"]),
        mesh=mesh,
        in_specs=placed,
        out_specs=(P(None, ("kv", "tp")), P("kv", "tp", None, None)),
        check_vma=False,
    )
```
